32 devices in a mesh: dp: 4 (over y, x), kv: 4 (over z), tp: 2 (over core).
Axes of the slice: x: 2, y: 2, z: 4, core: 2. Of those that a mesh axis runs over, the one named last changes fastest.
Arguments:
- hidden: bfloat16 [96, 2, 2048], P('dp', 'tp', 'kv'), may hold values from -6 to 6
- lengths: int32 [32], P('dp'), may hold values from 1 to 3, 42 in all
- state: float32 [32, 16, 128, 128], P(('dp', 'kv', 'tp')), may hold values from -6 to 6
- attn_gain: float32 [4096], replicated, may hold values from 0.1 to 1.9
- w_query: bfloat16 [4096, 2048], P(None, ('kv', 'tp')), may hold values from -0.09375 to 0.09375
- w_key: bfloat16 [4096, 2048], P(None, ('kv', 'tp')), may hold values from -0.09375 to 0.09375
- w_value: bfloat16 [4096, 2048], P(None, ('kv', 'tp')), may hold values from -0.09375 to 0.09375
- w_outgate: bfloat16 [4096, 2048], P(None, ('kv', 'tp')), may hold values from -0.09375 to 0.09375
- w_beta: bfloat16 [4096, 16], replicated, may hold values from -0.09375 to 0.09375
- w_decay: bfloat16 [4096, 16], replicated, may hold values from -0.09375 to 0.09375
- head_decay_rate: float32 [16], replicated, may hold values from 0.02 to 2
- decay_bias: float32 [16], replicated, may hold values from -3 to 1
- head_gain: float32 [128], replicated, may hold values from 0.1 to 1.9
- w_proj: bfloat16 [2048, 2, 2048], P(None, 'tp', 'kv'), may hold values from -0.125 to 0.125
- ffn_gain: float32 [4096], replicated, may hold values from 0.1 to 1.9
- w_gate: bfloat16 [4096, 11264], P('tp', 'kv'), may hold values from -0.09375 to 0.09375
- w_up: bfloat16 [4096, 11264], P('tp', 'kv'), may hold values from -0.09375 to 0.09375
- w_down: bfloat16 [11264, 4096], P('kv', 'tp'), may hold values from -0.078125 to 0.078125
Outputs:
- mixed: bfloat16 [96, 2, 2048], P('dp', 'tp', 'kv')
- new_state: float32 [32, 16, 128, 128], P(('dp', 'kv', 'tp'))
The draws below stay inside these ranges and needn't reach their ends.
Inputs may be any that keep to these rules, and one draw needn't show every extreme that they name: lengths sum to 42; some sequence has 3.
All inputs are finite; a program needn't handle non-finite values. No bound on the sum of `lengths` on one device may be relied on, other than what follows from the above.
Results may differ from the reference program's by a relative error of at most 0.015.
Values may be sent and summed in bfloat16 or wider, within the bound.
A program may use at most 128 MiB of HBM per device.

```python
import math
import jax
import jax.numpy as jnp
import numpy as np
from jax import lax

D = 4096
HEADS = 16
HEAD = 128
FF = 11264
SLOTS = 3
HD = 2048
DH = 2048
SEQS = 32
TOKENS = 96
LIVE = 42
N_TP = 2


def strengthened(result, rng, source, target, shards_of, factor):
    owner, partner = [(jnp.arange(result.shape[position]) // (result.shape[position] // shards_of)).reshape([-1 if axis == position else 1 for axis in range(result.ndim)]) for position in (source, target)]
    chosen = jax.random.permutation(rng, shards_of)[partner]
    strong = (owner == chosen) | (owner == (partner + shards_of // 2) % shards_of)
    return jnp.where(strong, factor * result, result)


def shard_levels(rng, shape, cuts, least, high):
    factor_of = 1.0
    for dim, blocks in cuts:
        heights = jax.random.uniform(jax.random.fold_in(jax.random.fold_in(rng, 6), dim), (blocks,), jnp.float32, least / len(cuts), high / len(cuts))
        factor_of = factor_of * jnp.repeat(jnp.exp(heights), shape[dim] // blocks).reshape((-1,) + (1,) * (len(shape) - 1 - dim))
    return factor_of


def split_up(amount, total, most, lean):
    portions = [(1 << 20) // math.isqrt(standing ** lean) + 1 for standing in range(2, amount + 1)]
    spare, holding = total - most - (amount - 1), [1] * (amount - 1)
    while spare > 0:
        movable = [i for i in range(amount - 1) if holding[i] < most]
        whole, budget = sum([portions[i] for i in movable]), spare
        for i in movable:
            extra = min(most - holding[i], max(1, budget * portions[i] // whole), spare)
            holding[i] = holding[i] + extra
            spare = spare - extra
    return np.array([most] + holding)


def ragged_sizes(stream_key, number_of, total, limit, lean):
    if number_of == 2:
        one = jax.random.randint(stream_key, (), max(1, total - limit), min(limit, total - 1) + 1)
        return jnp.stack([one, total - one])
    sizes = jnp.asarray(split_up(number_of, total, limit, lean), jnp.int32)
    couples = (number_of - 1) // 2
    donor, receiver = sizes[1:1 + 2 * couples:2], sizes[2:2 + 2 * couples:2]
    room = jnp.minimum(donor - 1, limit - receiver)
    moved = jax.random.randint(jax.random.fold_in(stream_key, 1), (couples,), 0, 1 << 20) % (room + 1)
    sizes = sizes.at[1:1 + 2 * couples:2].set(donor - moved).at[2:2 + 2 * couples:2].set(receiver + moved)
    return sizes[jax.random.permutation(jax.random.fold_in(stream_key, 2), number_of)]


def centred(rng, dims, spread, most, cuts=(), kind=jnp.bfloat16):
    values = spread * jax.random.normal(rng, dims, jnp.float32)
    if cuts:
        values = values * shard_levels(rng, dims, cuts, -0.22, 0.18)
    return jnp.clip(values, -most, most).astype(kind)


def noise_with(key, shape, width, most, cuts, heavy, kind=jnp.bfloat16):
    entries = width * jax.random.normal(key, shape, jnp.float32)
    if cuts:
        entries = entries * shard_levels(key, shape, cuts, -0.22, 0.18)
    return jnp.clip(strengthened(entries, jax.random.fold_in(key, 3), *heavy), -most, most).astype(kind)


def setup_inputs(seed: int = 0) -> dict:
    arg_keys = jax.random.split(jax.random.key(seed), 19)
    return {
        "hidden": centred(arg_keys[0], (TOKENS, N_TP, DH), 1.0, 6.0, ((0, 4), (1, 2), (2, 4))),
        "lengths": ragged_sizes(arg_keys[1], SEQS, LIVE, SLOTS, 2).astype(jnp.int32),
        "state": centred(arg_keys[2], (SEQS, HEADS, HEAD, HEAD), 1.0, 6.0, ((0, 32),), jnp.float32),
        "attn_gain": jnp.clip(1.0 + 0.18 * jax.random.normal(arg_keys[3], (D,), jnp.float32), 0.1, 1.9),
        "w_query": centred(arg_keys[4], (D, HD), D ** -0.5, 0.09375, ((1, 8),)),
        "w_key": centred(arg_keys[5], (D, HD), D ** -0.5, 0.09375, ((1, 8),)),
        "w_value": centred(arg_keys[6], (D, HD), D ** -0.5, 0.09375, ((1, 8),)),
        "w_outgate": centred(arg_keys[7], (D, HD), D ** -0.5, 0.09375, ((1, 8),)),
        "w_beta": centred(arg_keys[8], (D, HEADS), D ** -0.5, 0.09375),
        "w_decay": centred(arg_keys[9], (D, HEADS), D ** -0.5, 0.09375),
        "head_decay_rate": jnp.clip(jnp.exp(jax.random.uniform(arg_keys[10], (HEADS,), jnp.float32, math.log(0.02), math.log(2.0))), 0.02, 2.0),
        "decay_bias": jnp.clip(jax.random.uniform(arg_keys[11], (HEADS,), jnp.float32, -3.0, 1.0), -3.0, 1.0),
        "head_gain": jnp.clip(1.0 + 0.18 * jax.random.normal(arg_keys[12], (HEAD,), jnp.float32), 0.1, 1.9),
        "w_proj": centred(arg_keys[13], (HD, N_TP, DH), HD ** -0.5, 0.125, ((1, 2), (2, 4))),
        "ffn_gain": jnp.clip(1.0 + 0.18 * jax.random.normal(arg_keys[14], (D,), jnp.float32), 0.1, 1.9),
        "w_gate": centred(arg_keys[15], (D, FF), D ** -0.5, 0.09375, ((0, 2), (1, 4))),
        "w_up": centred(arg_keys[16], (D, FF), D ** -0.5, 0.09375, ((0, 2), (1, 4))),
        "w_down": noise_with(arg_keys[17], (FF, D), FF ** -0.5, 0.078125, ((0, 4), (1, 2)), (0, 1, 4, 2.0)),
    }


EPS = 1e-06

def recur(loop_carry, query_vector, key, value, beta, logdecay):
    query_scale = query_vector.shape[-1] ** (-0.5)
    output_rows = []
    for state_slot in range(query_vector.shape[0]):
        loop_carry = loop_carry * jnp.exp(logdecay[state_slot])[:, None, None]
        recalled_value = jnp.einsum('jtu,jt->ju', loop_carry, key[state_slot], precision=lax.Precision.HIGHEST)
        change = beta[state_slot][:, None] * (value[state_slot] - recalled_value)
        loop_carry = loop_carry + key[state_slot][:, :, None] * change[:, None, :]
        output_rows.append(jnp.einsum('jtu,jt->ju', loop_carry, query_vector[state_slot], precision=lax.Precision.HIGHEST) * query_scale)
    return (loop_carry, jnp.stack(output_rows))

def unit_rows(values):
    return values * lax.rsqrt(lax.optimization_barrier(jnp.sum(values * values, axis=-1, keepdims=True)) + EPS)

def reference(hidden, lengths, state, attn_gain, w_query, w_key, w_value, w_outgate, w_beta, w_decay, head_decay_rate, decay_bias, head_gain, w_proj, ffn_gain, w_gate, w_up, w_down):
    seqs = state.shape[0]
    heads = state.shape[1]
    head = state.shape[2]
    layout = hidden.shape
    flat = hidden.reshape(layout[0], -1)
    proj_flat = w_proj.reshape(w_proj.shape[0], -1)
    live = (jnp.arange(SLOTS)[None, :] < lengths[:, None]).astype(jnp.float32).reshape(-1)
    xf = flat.astype(jnp.float32)
    normed = (xf * lax.rsqrt(lax.optimization_barrier(jnp.mean(xf * xf, axis=1, keepdims=True)) + EPS) * attn_gain).astype(jnp.bfloat16)
    query_vector = jnp.dot(normed, w_query, preferred_element_type=jnp.float32).astype(jnp.bfloat16)
    key = jnp.dot(normed, w_key, preferred_element_type=jnp.float32).astype(jnp.bfloat16)
    value = jnp.dot(normed, w_value, preferred_element_type=jnp.float32).astype(jnp.bfloat16)
    outgate = jnp.dot(normed, w_outgate, preferred_element_type=jnp.float32).astype(jnp.bfloat16)
    beta = live[:, None] * jax.nn.sigmoid(jnp.dot(normed, w_beta, preferred_element_type=jnp.float32))
    pre = jnp.dot(normed, w_decay, preferred_element_type=jnp.float32)
    logdecay = -live[:, None] * head_decay_rate * jax.nn.softplus(pre + decay_bias)
    shape = (seqs, SLOTS, heads, head)
    q_all = unit_rows(query_vector.astype(jnp.float32).reshape(shape))
    k_all = unit_rows(key.astype(jnp.float32).reshape(shape))
    v_all = value.astype(jnp.float32).reshape(shape)
    beta = beta.reshape(seqs, SLOTS, heads)
    logdecay = logdecay.reshape(seqs, SLOTS, heads)
    new_state, out = lax.map(lambda item: recur(*item), (state, q_all, k_all, v_all, beta, logdecay))
    zf = outgate.astype(jnp.float32).reshape(shape)
    gated = out * lax.rsqrt(lax.optimization_barrier(jnp.mean(out * out, axis=-1, keepdims=True)) + EPS) * head_gain * jax.nn.silu(zf)
    gated = gated.reshape(seqs * SLOTS, heads * head).astype(jnp.bfloat16)
    stream = (xf + jnp.dot(gated, proj_flat, preferred_element_type=jnp.float32)).astype(jnp.bfloat16)
    sf = stream.astype(jnp.float32)
    fnormed = (sf * lax.rsqrt(lax.optimization_barrier(jnp.mean(sf * sf, axis=1, keepdims=True)) + EPS) * ffn_gain).astype(jnp.bfloat16)
    gate = jnp.dot(fnormed, w_gate, preferred_element_type=jnp.float32)
    upper = jnp.dot(fnormed, w_up, preferred_element_type=jnp.float32)
    inner = (jax.nn.silu(gate) * upper).astype(jnp.bfloat16)
    down = jnp.dot(inner, w_down, preferred_element_type=jnp.float32)
    mixed = ((sf + down) * live[:, None]).astype(jnp.bfloat16)
    return (mixed.reshape(layout), new_state)
```

```python
import functools

import jax
import jax.numpy as jnp
from jax import lax
from jax.experimental import pallas as pl
from jax.experimental.pallas import tpu as pltpu
from jax.sharding import PartitionSpec as P

D = 4096
HEADS = 16
HEAD = 128
SLOTS = 3


EPS = 1e-06


def recur(loop_carry, query_vector, key, value, beta, logdecay):
    query_scale = query_vector.shape[-1] ** (-0.5)
    output_rows = []
    for state_slot in range(query_vector.shape[0]):
        loop_carry = loop_carry * jnp.exp(logdecay[state_slot])[:, None, None]
        recalled_value = jnp.einsum(
            "jtu,jt->ju", loop_carry, key[state_slot], precision=lax.Precision.HIGHEST
        )
        change = beta[state_slot][:, None] * (value[state_slot] - recalled_value)
        loop_carry = loop_carry + key[state_slot][:, :, None] * change[:, None, :]
        output_rows.append(
            jnp.einsum(
                "jtu,jt->ju", loop_carry, query_vector[state_slot], precision=lax.Precision.HIGHEST
            )
            * query_scale
        )
    return (loop_carry, jnp.stack(output_rows))


def unit_rows(values):
    return values * lax.rsqrt(jnp.sum(values * values, axis=-1, keepdims=True) + EPS)


def local(
    hidden,
    lengths,
    state,
    attn_gain,
    w_query,
    w_key,
    w_value,
    w_outgate,
    w_beta,
    w_decay,
    head_decay_rate,
    decay_bias,
    head_gain,
    w_proj,
    ffn_gain,
    w_gate,
    w_up,
    w_down,
):
    rank = lax.axis_index(("kv", "tp"))
    core = lax.axis_index("tp")
    own = state.shape[0]
    own_rows = own * SLOTS
    row_total = hidden.shape[0]
    piece_cols = hidden.shape[2]
    half_cols = piece_cols * lax.axis_size("kv")
    live = (jnp.arange(SLOTS)[None, :] < lengths[:, None]).astype(jnp.float32).reshape(-1)
    own_lengths = lax.dynamic_slice_in_dim(lengths, rank * own, own)
    own_live = (jnp.arange(SLOTS)[None, :] < own_lengths[:, None]).astype(jnp.float32).reshape(-1)
    half_rows = lax.all_gather(hidden, "kv", axis=2, tiled=True)
    whole = lax.all_gather(half_rows, "tp", axis=1, tiled=True).reshape(row_total, -1)
    xf = whole.astype(jnp.float32)
    normed = (xf * lax.rsqrt(jnp.mean(xf * xf, axis=1, keepdims=True) + EPS) * attn_gain).astype(
        jnp.bfloat16
    )
    projected = jnp.stack(
        [
            jnp.dot(normed, weight, preferred_element_type=jnp.float32)
            for weight in (w_query, w_key, w_value, w_outgate)
        ],
        axis=1,
    ).astype(jnp.bfloat16)
    mine = lax.all_to_all(projected, ("kv", "tp"), split_axis=0, concat_axis=2, tiled=True)
    own_normed = lax.dynamic_slice_in_dim(normed, rank * own_rows, own_rows, 0)
    beta = own_live[:, None] * jax.nn.sigmoid(
        jnp.dot(own_normed, w_beta, preferred_element_type=jnp.float32)
    )
    pre = jnp.dot(own_normed, w_decay, preferred_element_type=jnp.float32)
    logdecay = -own_live[:, None] * head_decay_rate * jax.nn.softplus(pre + decay_bias)
    shape = (own, SLOTS, HEADS, HEAD)
    q_own = unit_rows(mine[:, 0].astype(jnp.float32).reshape(shape))
    k_own = unit_rows(mine[:, 1].astype(jnp.float32).reshape(shape))
    v_own = mine[:, 2].astype(jnp.float32).reshape(shape)
    zf = mine[:, 3].astype(jnp.float32).reshape(shape)
    new_state, out = jax.vmap(recur)(
        state,
        q_own,
        k_own,
        v_own,
        beta.reshape(own, SLOTS, HEADS),
        logdecay.reshape(own, SLOTS, HEADS),
    )
    gated = (
        out
        * lax.rsqrt(jnp.mean(out * out, axis=-1, keepdims=True) + EPS)
        * head_gain
        * jax.nn.silu(zf)
    )
    gated = gated.reshape(own_rows, HEADS * HEAD).astype(jnp.bfloat16)
    proj_cols = w_proj.reshape(w_proj.shape[0], -1)
    mixer = jnp.dot(
        lax.all_gather(gated, ("kv", "tp"), axis=0, tiled=True),
        proj_cols,
        preferred_element_type=jnp.float32,
    )
    stream = (hidden.astype(jnp.float32) + mixer[:, None, :]).astype(jnp.bfloat16)
    sf = stream.astype(jnp.float32)
    half_stream = lax.all_gather(stream, "kv", axis=2, tiled=True)[:, 0, :]
    hf = half_stream.astype(jnp.float32)
    squares = lax.psum(jnp.sum(hf * hf, axis=1), "tp")
    gain_half = lax.dynamic_slice_in_dim(ffn_gain, core * half_cols, half_cols)
    fnormed = (hf * lax.rsqrt(squares / D + EPS)[:, None] * gain_half).astype(jnp.bfloat16)
    gate_part = jnp.dot(fnormed, w_gate, preferred_element_type=jnp.float32)
    up_part = jnp.dot(fnormed, w_up, preferred_element_type=jnp.float32)
    gate, upper = (
        lax.psum(gate_part.astype(jnp.bfloat16), "tp").astype(jnp.float32),
        lax.psum(up_part.astype(jnp.bfloat16), "tp").astype(jnp.float32),
    )
    inner = (jax.nn.silu(gate) * upper).astype(jnp.bfloat16)
    partial_down = jnp.dot(inner, w_down, preferred_element_type=jnp.float32)[:, None, :]
    down = lax.psum_scatter(partial_down, "kv", scatter_dimension=2, tiled=True)
    mixed = ((sf + down) * live[:, None, None]).astype(jnp.bfloat16)
    return (mixed, new_state)


def layer_kernel(
    nk,
    hidden,
    lengths,
    state_hbm,
    attn_gain,
    wq_hbm,
    wk_hbm,
    wv_hbm,
    wz_hbm,
    wb_hbm,
    wd_hbm,
    rate,
    bias,
    head_gain,
    wp_hbm,
    ffn_gain,
    wg_hbm,
    wu_hbm,
    wdn_hbm,
    mixed,
    state_out,
    w_all,
    w_p,
    w_g,
    w_u,
    w_dn,
    w_bd,
    st,
    hx,
    acc,
    blocks,
    scale,
    px,
    rx,
    flat,
    qk,
    qkt,
    outs,
    gx,
    rg,
    flat2,
    sx,
    acc_g,
    acc_u,
    xs,
    rs,
    sq,
    rsq,
    dx,
    rd,
    w_sem,
    h_send,
    h_recv,
    p_send,
    p_recv,
    g_send,
    g_recv,
    s_send,
    s_recv,
    x_send,
    x_recv,
    d_send,
    d_recv,
):
    f32, bf16 = jnp.float32, jnp.bfloat16
    c = lax.axis_index("kv")
    t = lax.axis_index("tp")
    me = c * 2 + t
    group = 2 * nk
    rows, piece = hidden.shape
    cols = w_p.shape[0] // group
    seqs = rows // SLOTS
    width = group * piece
    turn = 1 - 2 * (c // max(nk // 2, 1))

    def near(i):
        return lax.rem(c + turn * i + nk, nk)

    def send(src, dst, ssem, rsem, kv, tp):
        copy = pltpu.make_async_remote_copy(
            src_ref=src,
            dst_ref=dst,
            send_sem=ssem,
            recv_sem=rsem,
            device_id={"kv": kv, "tp": tp},
            device_id_type=pl.DeviceIdType.MESH,
        )
        copy.start()
        return copy

    def arrived(ref, ssem, rsem):
        pltpu.make_async_remote_copy(
            src_ref=ref,
            dst_ref=ref,
            send_sem=ssem,
            recv_sem=rsem,
            device_id={"kv": c, "tp": 1 - t},
            device_id_type=pl.DeviceIdType.MESH,
        ).wait_recv()

    loads = []

    def load(src, dst):
        copy = pltpu.make_async_copy(src, dst, w_sem.at[len(loads)])
        copy.start()
        loads.append(copy)
        return copy

    own_off = pl.multiple_of((t * nk + c) * piece, piece)
    load_b = load(wb_hbm.at[:, pl.ds(own_off, piece)], w_bd.at[0:HEADS, :])
    load_d = load(wd_hbm.at[:, pl.ds(own_off, piece)], w_bd.at[HEADS : 2 * HEADS, :])
    w_bd[2 * HEADS :, :] = jnp.zeros((HEAD - 2 * HEADS, piece), bf16)
    load_proj = [load(w, w_all.at[j]) for j, w in enumerate((wq_hbm, wk_hbm, wv_hbm, wz_hbm))]
    load_state = load(state_hbm, st)
    load_p = load(wp_hbm, w_p)
    load_gu = [
        [load(a.at[pl.ds(near(i) * piece, piece), :], b.at[pl.ds(near(i) * piece, piece), :])
         for a, b in ((wg_hbm, w_g), (wu_hbm, w_u))]
        for i in range(nk)
    ]
    part = w_dn.shape[0] // 4
    load_dn = [
        load(wdn_hbm.at[pl.ds(i * part, part), :], w_dn.at[pl.ds(i * part, part), :])
        for i in range(4)
    ]

    barrier = pltpu.get_barrier_semaphore()
    others = [(i, j) for i in range(nk) for j in range(2) if i or j]
    for i, j in others:
        pl.semaphore_signal(
            barrier,
            inc=1,
            device_id={"kv": near(i), "tp": lax.rem(t + j, 2)},
            device_id_type=pl.DeviceIdType.MESH,
        )
    pl.semaphore_wait(barrier, len(others))

    sends = []
    own_slot = t * nk + c
    for i in range(1, nk):
        sends.append(
            send(hidden, hx.at[own_slot], h_send.at[i], h_recv.at[own_slot], near(i), t)
        )
    sends.append(send(hidden, hx.at[own_slot], h_send.at[0], h_recv.at[own_slot], c, 1 - t))

    def scaled(x, gain_ref, slot):
        gain = gain_ref[:, pl.ds(pl.multiple_of(slot * piece, piece), piece)]
        return (x * gain).astype(bf16)

    def proj(x, slot):
        return [
            jnp.dot(
                x,
                w_all[j, pl.ds(pl.multiple_of(slot * piece, piece), piece), :],
                preferred_element_type=f32,
            )
            for j in range(4)
        ]

    hf = hidden[...].astype(f32)
    xg = scaled(hf, attn_gain, own_slot)
    load_b.wait()
    load_d.wait()
    pbd = lax.dot_general(xg, w_bd[...], (((1,), (1,)), ((), ())), preferred_element_type=f32)
    for copy in load_proj:
        copy.wait()
    for j, value in enumerate(proj(xg, own_slot)):
        acc[:, j * cols : (j + 1) * cols] = value
    squares = jnp.sum(hf * hf, axis=1, keepdims=True)

    def slot_step(slot, squares):
        xf = hx[slot].astype(f32)
        for j, value in enumerate(proj(scaled(xf, attn_gain, slot), slot)):
            acc[:, j * cols : (j + 1) * cols] += value
        return squares + jnp.sum(xf * xf, axis=1, keepdims=True)

    for i in range(1, nk):
        slot = t * nk + near(i)
        arrived(hx.at[slot], h_send.at[0], h_recv.at[slot])
        sends.append(
            send(hx.at[slot], hx.at[slot], h_send.at[nk - 1 + i], h_recv.at[slot], c, 1 - t)
        )
    squares = lax.fori_loop(
        1, nk, lambda i, total: slot_step(t * nk + near(i), total), squares
    )

    def partner_step(i, total):
        slot = (1 - t) * nk + near(i)
        arrived(hx.at[slot], h_send.at[0], h_recv.at[slot])
        return slot_step(slot, total)

    squares = lax.fori_loop(0, nk, partner_step, squares)
    rms = lax.rsqrt(squares / width + EPS)
    scale[...] = jnp.broadcast_to(rms, (rows, HEAD))
    per = 4 * cols // HEAD
    for j in range(per):
        blocks[pl.ds(j, rows, stride=per), :] = acc[:, j * HEAD : (j + 1) * HEAD] * rms
    high = pbd.astype(bf16).astype(f32)
    low = pbd - high
    zero = jnp.zeros((2, HEAD), f32)
    span = SLOTS * per
    for g in range(group):
        at = slice(g * SLOTS, (g + 1) * SLOTS)
        px[g, 0:span, :] = blocks[g * span : (g + 1) * span, :].astype(bf16)
        px[g, span : span + 8, :] = jnp.concatenate([high[at], low[at], zero], axis=0).astype(bf16)
    for i, j in others:
        kv, tp = near(i), lax.rem(t + j, 2)
        sends.append(
            send(px.at[kv * 2 + tp], rx.at[me], p_send.at[i * 2 + j], p_recv.at[me], kv, tp)
        )
    rx[me] = px[me]
    tall = span + 8

    own_len = lengths[me]
    own_rms = [scale[pl.ds(me * SLOTS + s, 1), :] for s in range(SLOTS)]
    load_state.wait()
    for i, j in others:
        src = near(i) * 2 + lax.rem(t + j, 2)
        arrived(rx.at[src], p_send.at[0], p_recv.at[src])
    for g in range(group):
        flat[g * tall : (g + 1) * tall, :] = rx[g].astype(f32)
    hh = cols // HEAD

    def tile(s, p, h):
        return flat[pl.ds(s * per + p * hh + h, group, stride=tall), :]

    def unit(x):
        return x * lax.rsqrt(jnp.sum(x * x, axis=1, keepdims=True) + EPS)

    qk[...] = jnp.zeros_like(qk)
    for s in range(SLOTS):
        for h in range(hh):
            at = (s * hh + h) * group
            qk[at : at + group, :] = unit(tile(s, 0, h))
            at += SLOTS * HEADS
            qk[at : at + group, :] = unit(tile(s, 1, h))
    qkt[...] = qk[...].T
    betas, decays = [], []
    for s in range(SLOTS):
        pre = jnp.sum(
            flat[pl.ds(span + s, group, stride=tall), :]
            + flat[pl.ds(span + SLOTS + s, group, stride=tall), :],
            axis=0,
            keepdims=True,
        ) * own_rms[s]
        live = jnp.where(s < own_len, 1.0, 0.0).astype(f32)
        betas.append(live * jax.nn.sigmoid(pre[:, :HEADS]))
        arg = pre[:, HEADS : 2 * HEADS] + bias[...]
        soft = jnp.maximum(arg, 0.0) + jnp.log1p(jnp.exp(-jnp.abs(arg)))
        decays.append(jnp.exp(-live * rate[...] * soft))
    inv = HEAD**-0.5
    state_copies = []
    for src in range(group):
        for h in range(hh):
            n = src * hh + h
            S = st[n]
            for s in range(SLOTS):
                col = (s * hh + h) * group + src
                kc = qkt[:, col + SLOTS * HEADS : col + SLOTS * HEADS + 1]
                qc = qkt[:, col : col + 1]
                v = flat[src * tall + s * per + 2 * hh + h : src * tall + s * per + 2 * hh + h + 1, :]
                S = S * decays[s][:, n : n + 1]
                recalled = jnp.sum(S * kc, axis=0, keepdims=True)
                change = betas[s][:, n : n + 1] * (v - recalled)
                S = S + kc * change
                outs[col : col + 1, :] = jnp.sum(S * qc, axis=0, keepdims=True) * inv
            st[n] = S
    for s in range(SLOTS):
        for h in range(hh):
            at = (s * hh + h) * group
            o = outs[at : at + group, :]
            z = tile(s, 3, h)
            gated = (
                o
                * lax.rsqrt(jnp.mean(o * o, axis=1, keepdims=True) + EPS)
                * head_gain[...]
                * (z * jax.nn.sigmoid(z))
            )
            outs[at : at + group, :] = gated
    gx[...] = outs[...].astype(bf16)
    for i, j in others:
        kv, tp = near(i), lax.rem(t + j, 2)
        sends.append(send(gx, rg.at[me], g_send.at[i * 2 + j], g_recv.at[me], kv, tp))
    rg[me] = gx[...]
    state_copy = pltpu.make_async_copy(st, state_out, w_sem.at[len(loads)])
    state_copy.start()
    load_p.wait()
    for i, j in others:
        src = near(i) * 2 + lax.rem(t + j, 2)
        arrived(rg.at[src], g_send.at[0], g_recv.at[src])
    for g in range(group):
        flat2[g * SLOTS * HEADS : (g + 1) * SLOTS * HEADS, :] = rg[g].astype(f32)
    gall = jnp.concatenate(
        [
            flat2[pl.ds((n % hh) * group + n // hh, rows, stride=HEADS), :].astype(bf16)
            for n in range(HEADS)
        ],
        axis=1,
    )
    mixer = jnp.dot(gall, w_p[...], preferred_element_type=f32)
    sx[c] = (hf + mixer).astype(bf16)
    for i in range(1, nk):
        sends.append(send(sx.at[c], sx.at[c], s_send.at[i], s_recv.at[c], near(i), t))

    acc_g[...] = jnp.zeros_like(acc_g)
    acc_u[...] = jnp.zeros_like(acc_u)
    for i in range(nk):
        for copy in load_gu[i]:
            copy.wait()

    def ffn_step(i, total):
        slot = near(i)

        @pl.when(i > 0)
        def _():
            arrived(sx.at[slot], s_send.at[0], s_recv.at[slot])

        xf = sx[slot].astype(f32)
        x = scaled(xf, ffn_gain, t * nk + slot)
        at = pl.ds(pl.multiple_of(slot * piece, piece), piece)
        acc_g[...] += jnp.dot(x, w_g[at, :], preferred_element_type=f32)
        acc_u[...] += jnp.dot(x, w_u[at, :], preferred_element_type=f32)
        return total + jnp.sum(xf * xf, axis=1, keepdims=True)

    half = lax.fori_loop(0, nk, ffn_step, jnp.zeros((rows, 1), f32))
    sq[...] = jnp.broadcast_to(half, (rows, HEAD))
    xs[0] = acc_g[...].astype(bf16)
    xs[1] = acc_u[...].astype(bf16)
    x0 = send(sq, rsq, x_send.at[0], x_recv.at[0], c, 1 - t)
    x1 = send(xs, rs, x_send.at[1], x_recv.at[1], c, 1 - t)
    sends += [x0, x1]
    for copy in load_dn:
        copy.wait()
    x0.wait_recv()
    x1.wait_recv()
    fr = lax.rsqrt((half + rsq[:, 0:1]) / width + EPS)
    gate = (acc_g[...] + rs[0].astype(f32)) * fr
    upper = (acc_u[...] + rs[1].astype(f32)) * fr
    inner = (gate * jax.nn.sigmoid(gate) * upper).astype(bf16)
    xs_inner = inner

    def down(slot):
        at = pl.ds(pl.multiple_of(slot * piece, piece), piece)
        return jnp.dot(xs_inner, w_dn[:, at], preferred_element_type=f32)

    for i in range(nk - 1, 0, -1):
        slot = near(i)
        dx[i] = down(slot).astype(bf16)
        sends.append(send(dx.at[i], rd.at[c], d_send.at[i], d_recv.at[c], slot, t))
    total = sx[c].astype(f32) + down(c)
    row = lax.broadcasted_iota(jnp.int32, (rows, piece), 0)
    live = jnp.zeros((rows, piece), f32)
    for n in range(seqs):
        hit = (row >= n * SLOTS) & (row < n * SLOTS + lengths[n])
        live = jnp.where(hit, 1.0, live)
    for i in range(1, nk):
        slot = near(i)
        arrived(rd.at[slot], d_send.at[0], d_recv.at[slot])
        total = total + rd[slot].astype(f32)
    mixed[...] = (total * live).astype(bf16)
    for copy in sends:
        copy.wait_send()
    state_copy.wait()


def fused(
    nk,
    hidden,
    lengths,
    state,
    attn_gain,
    w_query,
    w_key,
    w_value,
    w_outgate,
    w_beta,
    w_decay,
    head_decay_rate,
    decay_bias,
    head_gain,
    w_proj,
    ffn_gain,
    w_gate,
    w_up,
    w_down,
):
    f32, bf16 = jnp.float32, jnp.bfloat16
    rows, _, piece = hidden.shape
    group = 2 * nk
    depth, cols = w_query.shape
    hd = w_proj.shape[0]
    half, ff = w_gate.shape
    per = 4 * cols // HEAD
    tall = SLOTS * per + 8
    vmem = pl.BlockSpec(memory_space=pltpu.VMEM)
    smem = pl.BlockSpec(memory_space=pltpu.SMEM)
    hbm = pl.BlockSpec(memory_space=pl.ANY)
    dma = pltpu.SemaphoreType.DMA
    mixed, new_state = pl.pallas_call(
        functools.partial(layer_kernel, nk),
        out_shape=(
            jax.ShapeDtypeStruct((rows, piece), bf16),
            jax.ShapeDtypeStruct(state.shape[1:], f32),
        ),
        in_specs=[vmem, smem, hbm, vmem] + [hbm] * 6 + [vmem] * 3 + [hbm, vmem] + [hbm] * 3,
        out_specs=(vmem, hbm),
        scratch_shapes=[
            pltpu.VMEM((4, depth, cols), bf16),
            pltpu.VMEM((hd, piece), bf16),
            pltpu.VMEM((half, ff), bf16),
            pltpu.VMEM((half, ff), bf16),
            pltpu.VMEM(w_down.shape, bf16),
            pltpu.VMEM((HEAD, piece), bf16),
            pltpu.VMEM(state.shape[1:], f32),
            pltpu.VMEM((group, rows, piece), bf16),
            pltpu.VMEM((rows, 4 * cols), f32),
            pltpu.VMEM((rows * per, HEAD), f32),
            pltpu.VMEM((rows, HEAD), f32),
            pltpu.VMEM((group, tall, HEAD), bf16),
            pltpu.VMEM((group, tall, HEAD), bf16),
            pltpu.VMEM((group * tall, HEAD), f32),
            pltpu.VMEM((HEAD, HEAD), f32),
            pltpu.VMEM((HEAD, HEAD), f32),
            pltpu.VMEM((SLOTS * HEADS, HEAD), f32),
            pltpu.VMEM((SLOTS * HEADS, HEAD), bf16),
            pltpu.VMEM((group, SLOTS * HEADS, HEAD), bf16),
            pltpu.VMEM((group * SLOTS * HEADS, HEAD), f32),
            pltpu.VMEM((nk, rows, piece), bf16),
            pltpu.VMEM((rows, ff), f32),
            pltpu.VMEM((rows, ff), f32),
            pltpu.VMEM((2, rows, ff), bf16),
            pltpu.VMEM((2, rows, ff), bf16),
            pltpu.VMEM((rows, HEAD), f32),
            pltpu.VMEM((rows, HEAD), f32),
            pltpu.VMEM((nk, rows, piece), bf16),
            pltpu.VMEM((nk, rows, piece), bf16),
            dma((13 + 2 * nk,)),
            dma((group,)),
            dma((group,)),
            dma((group,)),
            dma((group,)),
            dma((group,)),
            dma((group,)),
            dma((nk,)),
            dma((nk,)),
            dma((2,)),
            dma((2,)),
            dma((nk,)),
            dma((nk,)),
        ],
        compiler_params=pltpu.CompilerParams(
            collective_id=0, has_side_effects=True, vmem_limit_bytes=62 * 2**20
        ),
        name="layer",
    )(
        hidden.reshape(rows, piece),
        lengths,
        state.reshape(state.shape[1:]),
        attn_gain.reshape(1, -1),
        w_query,
        w_key,
        w_value,
        w_outgate,
        w_beta.T,
        w_decay.T,
        head_decay_rate.reshape(1, -1),
        decay_bias.reshape(1, -1),
        head_gain.reshape(1, -1),
        w_proj.reshape(hd, piece),
        ffn_gain.reshape(1, -1),
        w_gate,
        w_up,
        w_down,
    )
    return mixed.reshape(hidden.shape), new_state.reshape(state.shape)


def dispatch(nk, nt, hidden, lengths, state, *rest):
    piece, cols = hidden.shape[2], rest[1].shape[1]
    fits = (
        nt == 2
        and nk == 4
        and state.shape[0] == 1
        and hidden.shape[0] % 8 == 0
        and piece % HEAD == 0
        and cols % HEAD == 0
        and rest[-3].shape[1] % HEAD == 0
    )
    plan = functools.partial(fused, nk) if fits else local
    return plan(hidden, lengths, state, *rest)


def solution(mesh):
    in_specs = (
        P("dp", "tp", "kv"),
        P("dp"),
        P(("dp", "kv", "tp"), None, None, None),
        P(),
        P(None, ("kv", "tp")),
        P(None, ("kv", "tp")),
        P(None, ("kv", "tp")),
        P(None, ("kv", "tp")),
        P(),
        P(),
        P(),
        P(),
        P(),
        P(None, "tp", "kv"),
        P(),
        P("tp", "kv"),
        P("tp", "kv"),
        P("kv", "tp"),
    )
    out_specs = (P("dp", "tp", "kv"), P(("dp", "kv", "tp"), None, None, None))
    plan = functools.partial(dispatch, mesh.shape["kv"], mesh.shape["tp"])
    return jax.shard_map(plan, mesh=mesh, in_specs=in_specs, out_specs=out_specs, check_vma=False)
```

```python
import functools

import jax
import jax.numpy as jnp
from jax import lax
from jax.experimental import pallas as pl
from jax.experimental.pallas import tpu as pltpu
from jax.sharding import PartitionSpec as P

D = 4096
HEADS = 16
HEAD = 128
SLOTS = 3


EPS = 1e-06


def recur(loop_carry, query_vector, key, value, beta, logdecay):
    query_scale = query_vector.shape[-1] ** (-0.5)
    output_rows = []
    for state_slot in range(query_vector.shape[0]):
        loop_carry = loop_carry * jnp.exp(logdecay[state_slot])[:, None, None]
        recalled_value = jnp.einsum(
            "jtu,jt->ju", loop_carry, key[state_slot], precision=lax.Precision.HIGHEST
        )
        change = beta[state_slot][:, None] * (value[state_slot] - recalled_value)
        loop_carry = loop_carry + key[state_slot][:, :, None] * change[:, None, :]
        output_rows.append(
            jnp.einsum(
                "jtu,jt->ju", loop_carry, query_vector[state_slot], precision=lax.Precision.HIGHEST
            )
            * query_scale
        )
    return (loop_carry, jnp.stack(output_rows))


def unit_rows(values):
    return values * lax.rsqrt(jnp.sum(values * values, axis=-1, keepdims=True) + EPS)


def local(
    hidden,
    lengths,
    state,
    attn_gain,
    w_query,
    w_key,
    w_value,
    w_outgate,
    w_beta,
    w_decay,
    head_decay_rate,
    decay_bias,
    head_gain,
    w_proj,
    ffn_gain,
    w_gate,
    w_up,
    w_down,
):
    rank = lax.axis_index(("kv", "tp"))
    core = lax.axis_index("tp")
    own = state.shape[0]
    own_rows = own * SLOTS
    row_total = hidden.shape[0]
    piece_cols = hidden.shape[2]
    half_cols = piece_cols * lax.axis_size("kv")
    live = (jnp.arange(SLOTS)[None, :] < lengths[:, None]).astype(jnp.float32).reshape(-1)
    own_lengths = lax.dynamic_slice_in_dim(lengths, rank * own, own)
    own_live = (jnp.arange(SLOTS)[None, :] < own_lengths[:, None]).astype(jnp.float32).reshape(-1)
    half_rows = lax.all_gather(hidden, "kv", axis=2, tiled=True)
    whole = lax.all_gather(half_rows, "tp", axis=1, tiled=True).reshape(row_total, -1)
    xf = whole.astype(jnp.float32)
    normed = (xf * lax.rsqrt(jnp.mean(xf * xf, axis=1, keepdims=True) + EPS) * attn_gain).astype(
        jnp.bfloat16
    )
    projected = jnp.stack(
        [
            jnp.dot(normed, weight, preferred_element_type=jnp.float32)
            for weight in (w_query, w_key, w_value, w_outgate)
        ],
        axis=1,
    ).astype(jnp.bfloat16)
    mine = lax.all_to_all(projected, ("kv", "tp"), split_axis=0, concat_axis=2, tiled=True)
    own_normed = lax.dynamic_slice_in_dim(normed, rank * own_rows, own_rows, 0)
    beta = own_live[:, None] * jax.nn.sigmoid(
        jnp.dot(own_normed, w_beta, preferred_element_type=jnp.float32)
    )
    pre = jnp.dot(own_normed, w_decay, preferred_element_type=jnp.float32)
    logdecay = -own_live[:, None] * head_decay_rate * jax.nn.softplus(pre + decay_bias)
    shape = (own, SLOTS, HEADS, HEAD)
    q_own = unit_rows(mine[:, 0].astype(jnp.float32).reshape(shape))
    k_own = unit_rows(mine[:, 1].astype(jnp.float32).reshape(shape))
    v_own = mine[:, 2].astype(jnp.float32).reshape(shape)
    zf = mine[:, 3].astype(jnp.float32).reshape(shape)
    new_state, out = jax.vmap(recur)(
        state,
        q_own,
        k_own,
        v_own,
        beta.reshape(own, SLOTS, HEADS),
        logdecay.reshape(own, SLOTS, HEADS),
    )
    gated = (
        out
        * lax.rsqrt(jnp.mean(out * out, axis=-1, keepdims=True) + EPS)
        * head_gain
        * jax.nn.silu(zf)
    )
    gated = gated.reshape(own_rows, HEADS * HEAD).astype(jnp.bfloat16)
    proj_cols = w_proj.reshape(w_proj.shape[0], -1)
    mixer = jnp.dot(
        lax.all_gather(gated, ("kv", "tp"), axis=0, tiled=True),
        proj_cols,
        preferred_element_type=jnp.float32,
    )
    stream = (hidden.astype(jnp.float32) + mixer[:, None, :]).astype(jnp.bfloat16)
    sf = stream.astype(jnp.float32)
    half_stream = lax.all_gather(stream, "kv", axis=2, tiled=True)[:, 0, :]
    hf = half_stream.astype(jnp.float32)
    squares = lax.psum(jnp.sum(hf * hf, axis=1), "tp")
    gain_half = lax.dynamic_slice_in_dim(ffn_gain, core * half_cols, half_cols)
    fnormed = (hf * lax.rsqrt(squares / D + EPS)[:, None] * gain_half).astype(jnp.bfloat16)
    gate_part = jnp.dot(fnormed, w_gate, preferred_element_type=jnp.float32)
    up_part = jnp.dot(fnormed, w_up, preferred_element_type=jnp.float32)
    gate, upper = (
        lax.psum(gate_part.astype(jnp.bfloat16), "tp").astype(jnp.float32),
        lax.psum(up_part.astype(jnp.bfloat16), "tp").astype(jnp.float32),
    )
    inner = (jax.nn.silu(gate) * upper).astype(jnp.bfloat16)
    partial_down = jnp.dot(inner, w_down, preferred_element_type=jnp.float32)[:, None, :]
    down = lax.psum_scatter(partial_down, "kv", scatter_dimension=2, tiled=True)
    mixed = ((sf + down) * live[:, None, None]).astype(jnp.bfloat16)
    return (mixed, new_state)


def layer_kernel(
    nk,
    hidden,
    lengths_hbm,
    state_hbm,
    attn_gain_hbm,
    wq_hbm,
    wk_hbm,
    wv_hbm,
    wz_hbm,
    wb_hbm,
    wd_hbm,
    rate_hbm,
    bias_hbm,
    head_gain_hbm,
    wp_hbm,
    ffn_gain_hbm,
    wg_hbm,
    wu_hbm,
    wdn_hbm,
    mixed,
    state_out,
    w_all,
    w_p,
    w_g,
    w_u,
    w_dn,
    w_bd,
    st,
    hx,
    acc,
    blocks,
    scale,
    px,
    rx,
    flat,
    qk,
    qkt,
    outs,
    gx,
    rg,
    flat2,
    sx,
    acc_g,
    acc_u,
    xs,
    rs,
    sq,
    rsq,
    dx,
    rd,
    lengths,
    attn_gain,
    ffn_gain,
    rate,
    bias,
    head_gain,
    w_sem,
    h_send,
    h_recv,
    p_send,
    p_recv,
    g_send,
    g_recv,
    s_send,
    s_recv,
    x_send,
    x_recv,
    d_send,
    d_recv,
):
    f32, bf16 = jnp.float32, jnp.bfloat16
    c = lax.axis_index("kv")
    t = lax.axis_index("tp")
    me = c * 2 + t
    group = 2 * nk
    rows, piece = hidden.shape
    cols = w_p.shape[0] // group
    seqs = rows // SLOTS
    width = group * piece
    turn = 1 - 2 * (c // max(nk // 2, 1))

    def near(i):
        return lax.rem(c + turn * i + nk, nk)

    def send(src, dst, ssem, rsem, kv, tp):
        copy = pltpu.make_async_remote_copy(
            src_ref=src,
            dst_ref=dst,
            send_sem=ssem,
            recv_sem=rsem,
            device_id={"kv": kv, "tp": tp},
            device_id_type=pl.DeviceIdType.MESH,
        )
        copy.start()
        return copy

    def arrived(ref, ssem, rsem):
        pltpu.make_async_remote_copy(
            src_ref=ref,
            dst_ref=ref,
            send_sem=ssem,
            recv_sem=rsem,
            device_id={"kv": c, "tp": 1 - t},
            device_id_type=pl.DeviceIdType.MESH,
        ).wait_recv()

    barrier = pltpu.get_barrier_semaphore()
    others = [(i, j) for i in reversed(range(nk)) for j in range(2) if i or j]
    for i, j in others:
        pl.semaphore_signal(
            barrier,
            inc=1,
            device_id={"kv": near(i), "tp": lax.rem(t + j, 2)},
            device_id_type=pl.DeviceIdType.MESH,
        )
    loads = []

    def load(src, dst):
        copy = pltpu.make_async_copy(src, dst, w_sem.at[len(loads)])
        copy.start()
        loads.append(copy)
        return copy

    own_slot = t * nk + c
    own_off = pl.multiple_of(own_slot * piece, piece)
    load_hidden = load(hidden, hx.at[own_slot])
    load_small = [
        load(a, b)
        for a, b in (
            (attn_gain_hbm, attn_gain),
            (lengths_hbm, lengths),
            (ffn_gain_hbm, ffn_gain),
            (rate_hbm, rate),
            (bias_hbm, bias),
            (head_gain_hbm, head_gain),
        )
    ]
    load_b = load(wb_hbm.at[:, pl.ds(own_off, piece)], w_bd.at[0:HEADS, :])
    load_d = load(wd_hbm.at[:, pl.ds(own_off, piece)], w_bd.at[HEADS : 2 * HEADS, :])
    w_bd[2 * HEADS :, :] = jnp.zeros((HEAD - 2 * HEADS, piece), bf16)
    load_proj = [load(w, w_all.at[j]) for j, w in enumerate((wq_hbm, wk_hbm, wv_hbm, wz_hbm))]
    load_state = load(state_hbm, st)
    load_p = load(wp_hbm, w_p)
    load_gu = [
        [load(a.at[pl.ds(near(i) * piece, piece), :], b.at[pl.ds(near(i) * piece, piece), :])
         for a, b in ((wg_hbm, w_g), (wu_hbm, w_u))]
        for i in range(nk)
    ]
    part = w_dn.shape[0] // 4
    load_dn = [
        load(wdn_hbm.at[pl.ds(i * part, part), :], w_dn.at[pl.ds(i * part, part), :])
        for i in range(4)
    ]

    sends = []
    load_hidden.wait()
    pl.semaphore_wait(barrier, len(others))

    mine = hx.at[own_slot]
    for i in reversed(range(1, nk)):
        sends.append(send(mine, mine, h_send.at[i], h_recv.at[own_slot], near(i), t))
    sends.append(send(mine, mine, h_send.at[0], h_recv.at[own_slot], c, 1 - t))

    def scaled(x, gain_ref, slot):
        gain = gain_ref[:, pl.ds(pl.multiple_of(slot * piece, piece), piece)]
        return (x * gain).astype(bf16)

    def proj(x, slot):
        return [
            jnp.dot(
                x,
                w_all[j, pl.ds(pl.multiple_of(slot * piece, piece), piece), :],
                preferred_element_type=f32,
            )
            for j in range(4)
        ]

    for copy in load_small:
        copy.wait()
    hf = hx[own_slot].astype(f32)
    xg = scaled(hf, attn_gain, own_slot)
    load_b.wait()
    load_d.wait()
    pbd = lax.dot_general(xg, w_bd[...], (((1,), (1,)), ((), ())), preferred_element_type=f32)
    for copy in load_proj:
        copy.wait()
    for j, value in enumerate(proj(xg, own_slot)):
        acc[:, j * cols : (j + 1) * cols] = value
    squares = jnp.sum(hf * hf, axis=1, keepdims=True)

    def slot_step(slot, squares):
        xf = hx[slot].astype(f32)
        for j, value in enumerate(proj(scaled(xf, attn_gain, slot), slot)):
            acc[:, j * cols : (j + 1) * cols] += value
        return squares + jnp.sum(xf * xf, axis=1, keepdims=True)

    for i in range(1, nk):
        slot = t * nk + near(i)
        arrived(hx.at[slot], h_send.at[0], h_recv.at[slot])
        sends.append(
            send(hx.at[slot], hx.at[slot], h_send.at[nk - 1 + i], h_recv.at[slot], c, 1 - t)
        )
        squares = slot_step(slot, squares)

    def partner_step(i, total):
        slot = (1 - t) * nk + near(i)
        arrived(hx.at[slot], h_send.at[0], h_recv.at[slot])
        return slot_step(slot, total)

    squares = lax.fori_loop(0, nk, partner_step, squares)
    rms = lax.rsqrt(squares / width + EPS)
    scale[...] = jnp.broadcast_to(rms, (rows, HEAD))
    per = 4 * cols // HEAD
    for j in range(per):
        blocks[pl.ds(j, rows, stride=per), :] = acc[:, j * HEAD : (j + 1) * HEAD] * rms
    high = pbd.astype(bf16).astype(f32)
    low = pbd - high
    zero = jnp.zeros((2, HEAD), f32)
    span = SLOTS * per
    for g in range(group):
        at = slice(g * SLOTS, (g + 1) * SLOTS)
        px[g, 0:span, :] = blocks[g * span : (g + 1) * span, :].astype(bf16)
        px[g, span : span + 8, :] = jnp.concatenate([high[at], low[at], zero], axis=0).astype(bf16)
    for i, j in others:
        kv, tp = near(i), lax.rem(t + j, 2)
        sends.append(
            send(px.at[kv * 2 + tp], rx.at[me], p_send.at[i * 2 + j], p_recv.at[me], kv, tp)
        )
    rx[me] = px[me]
    tall = span + 8

    own_len = lengths[me]
    own_rms = [scale[pl.ds(me * SLOTS + s, 1), :] for s in range(SLOTS)]
    load_state.wait()
    for i, j in others:
        src = near(i) * 2 + lax.rem(t + j, 2)
        arrived(rx.at[src], p_send.at[0], p_recv.at[src])
    for g in range(group):
        flat[g * tall : (g + 1) * tall, :] = rx[g].astype(f32)
    hh = cols // HEAD

    def tile(s, p, h):
        return flat[pl.ds(s * per + p * hh + h, group, stride=tall), :]

    def unit(x):
        return x * lax.rsqrt(jnp.sum(x * x, axis=1, keepdims=True) + EPS)

    qk[...] = jnp.zeros_like(qk)
    for s in range(SLOTS):
        for h in range(hh):
            at = (s * hh + h) * group
            qk[at : at + group, :] = unit(tile(s, 0, h))
            at += SLOTS * HEADS
            qk[at : at + group, :] = unit(tile(s, 1, h))
    qkt[...] = qk[...].T
    betas, decays = [], []
    for s in range(SLOTS):
        pre = jnp.sum(
            flat[pl.ds(span + s, group, stride=tall), :]
            + flat[pl.ds(span + SLOTS + s, group, stride=tall), :],
            axis=0,
            keepdims=True,
        ) * own_rms[s]
        live = jnp.where(s < own_len, 1.0, 0.0).astype(f32)
        betas.append(live * jax.nn.sigmoid(pre[:, :HEADS]))
        arg = pre[:, HEADS : 2 * HEADS] + bias[...]
        soft = jnp.maximum(arg, 0.0) + jnp.log1p(jnp.exp(-jnp.abs(arg)))
        decays.append(jnp.exp(-live * rate[...] * soft))
    inv = HEAD**-0.5
    state_copies = []
    for src in range(group):
        for h in range(hh):
            n = src * hh + h
            S = st[n]
            for s in range(SLOTS):
                col = (s * hh + h) * group + src
                kc = qkt[:, col + SLOTS * HEADS : col + SLOTS * HEADS + 1]
                qc = qkt[:, col : col + 1]
                v = flat[src * tall + s * per + 2 * hh + h : src * tall + s * per + 2 * hh + h + 1, :]
                S = S * decays[s][:, n : n + 1]
                recalled = jnp.sum(S * kc, axis=0, keepdims=True)
                change = betas[s][:, n : n + 1] * (v - recalled)
                S = S + kc * change
                outs[col : col + 1, :] = jnp.sum(S * qc, axis=0, keepdims=True) * inv
            state_out[n] = S
    for s in range(SLOTS):
        for h in range(hh):
            at = (s * hh + h) * group
            o = outs[at : at + group, :]
            z = tile(s, 3, h)
            gated = (
                o
                * lax.rsqrt(jnp.mean(o * o, axis=1, keepdims=True) + EPS)
                * head_gain[...]
                * (z * jax.nn.sigmoid(z))
            )
            outs[at : at + group, :] = gated
    gx[...] = outs[...].astype(bf16)
    for i, j in others:
        kv, tp = near(i), lax.rem(t + j, 2)
        sends.append(send(gx, rg.at[me], g_send.at[i * 2 + j], g_recv.at[me], kv, tp))
    rg[me] = gx[...]
    load_p.wait()
    for i, j in others:
        src = near(i) * 2 + lax.rem(t + j, 2)
        arrived(rg.at[src], g_send.at[0], g_recv.at[src])
    for g in range(group):
        flat2[g * SLOTS * HEADS : (g + 1) * SLOTS * HEADS, :] = rg[g].astype(f32)
    gall = jnp.concatenate(
        [
            flat2[pl.ds((n % hh) * group + n // hh, rows, stride=HEADS), :].astype(bf16)
            for n in range(HEADS)
        ],
        axis=1,
    )
    mixer = jnp.dot(gall, w_p[...], preferred_element_type=f32)
    sx[c] = (hf + mixer).astype(bf16)
    for i in reversed(range(1, nk)):
        sends.append(send(sx.at[c], sx.at[c], s_send.at[i], s_recv.at[c], near(i), t))

    acc_g[...] = jnp.zeros_like(acc_g)
    acc_u[...] = jnp.zeros_like(acc_u)
    for i in range(nk):
        for copy in load_gu[i]:
            copy.wait()

    def ffn_step(i, total):
        slot = near(i)

        @pl.when(i > 0)
        def _():
            arrived(sx.at[slot], s_send.at[0], s_recv.at[slot])

        xf = sx[slot].astype(f32)
        x = scaled(xf, ffn_gain, t * nk + slot)
        at = pl.ds(pl.multiple_of(slot * piece, piece), piece)
        acc_g[...] += jnp.dot(x, w_g[at, :], preferred_element_type=f32)
        acc_u[...] += jnp.dot(x, w_u[at, :], preferred_element_type=f32)
        return total + jnp.sum(xf * xf, axis=1, keepdims=True)

    half = lax.fori_loop(0, nk, ffn_step, jnp.zeros((rows, 1), f32))
    sq[...] = jnp.broadcast_to(half, (rows, HEAD))
    xs[0] = acc_g[...].astype(bf16)
    xs[1] = acc_u[...].astype(bf16)
    x0 = send(sq, rsq, x_send.at[0], x_recv.at[0], c, 1 - t)
    x1 = send(xs, rs, x_send.at[1], x_recv.at[1], c, 1 - t)
    sends += [x0, x1]
    for copy in load_dn:
        copy.wait()
    x0.wait_recv()
    x1.wait_recv()
    fr = lax.rsqrt((half + rsq[:, 0:1]) / width + EPS)
    gate = (acc_g[...] + rs[0].astype(f32)) * fr
    upper = (acc_u[...] + rs[1].astype(f32)) * fr
    inner = (gate * jax.nn.sigmoid(gate) * upper).astype(bf16)
    xs_inner = inner

    def down(slot):
        at = pl.ds(pl.multiple_of(slot * piece, piece), piece)
        return jnp.dot(xs_inner, w_dn[:, at], preferred_element_type=f32)

    for i in range(nk - 1, 0, -1):
        slot = near(i)
        dx[i] = down(slot).astype(bf16)
        sends.append(send(dx.at[i], rd.at[c], d_send.at[i], d_recv.at[c], slot, t))
    total = sx[c].astype(f32) + down(c)
    row = lax.broadcasted_iota(jnp.int32, (rows, piece), 0)
    live = jnp.zeros((rows, piece), f32)
    for n in range(seqs):
        hit = (row >= n * SLOTS) & (row < n * SLOTS + lengths[n])
        live = jnp.where(hit, 1.0, live)
    for i in range(1, nk):
        slot = near(i)
        arrived(rd.at[slot], d_send.at[0], d_recv.at[slot])
        total = total + rd[slot].astype(f32)
    mixed[...] = (total * live).astype(bf16)
    for copy in sends:
        copy.wait_send()


def write_kernel(a, b, a_out, b_out, sem):
    copies = [
        pltpu.make_async_copy(x, y, sem.at[n]) for n, (x, y) in enumerate(((b, b_out), (a, a_out)))
    ]
    for copy in copies:
        copy.start()
    for copy in copies:
        copy.wait()


def fused(
    nk,
    hidden,
    lengths,
    state,
    attn_gain,
    w_query,
    w_key,
    w_value,
    w_outgate,
    w_beta,
    w_decay,
    head_decay_rate,
    decay_bias,
    head_gain,
    w_proj,
    ffn_gain,
    w_gate,
    w_up,
    w_down,
):
    f32, bf16 = jnp.float32, jnp.bfloat16
    rows, _, piece = hidden.shape
    group = 2 * nk
    depth, cols = w_query.shape
    hd = w_proj.shape[0]
    half, ff = w_gate.shape
    per = 4 * cols // HEAD
    tall = SLOTS * per + 8
    vmem = pl.BlockSpec(memory_space=pltpu.VMEM)
    hbm = pl.BlockSpec(memory_space=pl.ANY)
    dma = pltpu.SemaphoreType.DMA
    mixed, new_state = pl.pallas_call(
        functools.partial(layer_kernel, nk),
        out_shape=(
            pltpu.VMEM((rows, piece), bf16),
            pltpu.VMEM(state.shape[1:], f32),
        ),
        in_specs=[hbm] * 18,
        out_specs=(vmem, vmem),
        scratch_shapes=[
            pltpu.VMEM((4, depth, cols), bf16),
            pltpu.VMEM((hd, piece), bf16),
            pltpu.VMEM((half, ff), bf16),
            pltpu.VMEM((half, ff), bf16),
            pltpu.VMEM(w_down.shape, bf16),
            pltpu.VMEM((HEAD, piece), bf16),
            pltpu.VMEM(state.shape[1:], f32),
            pltpu.VMEM((group, rows, piece), bf16),
            pltpu.VMEM((rows, 4 * cols), f32),
            pltpu.VMEM((rows * per, HEAD), f32),
            pltpu.VMEM((rows, HEAD), f32),
            pltpu.VMEM((group, tall, HEAD), bf16),
            pltpu.VMEM((group, tall, HEAD), bf16),
            pltpu.VMEM((group * tall, HEAD), f32),
            pltpu.VMEM((HEAD, HEAD), f32),
            pltpu.VMEM((HEAD, HEAD), f32),
            pltpu.VMEM((SLOTS * HEADS, HEAD), f32),
            pltpu.VMEM((SLOTS * HEADS, HEAD), bf16),
            pltpu.VMEM((group, SLOTS * HEADS, HEAD), bf16),
            pltpu.VMEM((group * SLOTS * HEADS, HEAD), f32),
            pltpu.VMEM((nk, rows, piece), bf16),
            pltpu.VMEM((rows, ff), f32),
            pltpu.VMEM((rows, ff), f32),
            pltpu.VMEM((2, rows, ff), bf16),
            pltpu.VMEM((2, rows, ff), bf16),
            pltpu.VMEM((rows, HEAD), f32),
            pltpu.VMEM((rows, HEAD), f32),
            pltpu.VMEM((nk, rows, piece), bf16),
            pltpu.VMEM((nk, rows, piece), bf16),
            pltpu.SMEM(lengths.shape, jnp.int32),
            pltpu.VMEM((1, 2 * half), f32),
            pltpu.VMEM((1, 2 * half), f32),
            pltpu.VMEM((1, HEADS), f32),
            pltpu.VMEM((1, HEADS), f32),
            pltpu.VMEM((1, HEAD), f32),
            dma((20 + 2 * nk,)),
            dma((group,)),
            dma((group,)),
            dma((group,)),
            dma((group,)),
            dma((group,)),
            dma((group,)),
            dma((nk,)),
            dma((nk,)),
            dma((2,)),
            dma((2,)),
            dma((nk,)),
            dma((nk,)),
        ],
        compiler_params=pltpu.CompilerParams(
            collective_id=0, has_side_effects=True, vmem_limit_bytes=60 * 2**20
        ),
        name="layer",
    )(
        hidden.reshape(rows, piece),
        lengths,
        state.reshape(state.shape[1:]),
        attn_gain.reshape(1, -1),
        w_query,
        w_key,
        w_value,
        w_outgate,
        w_beta.T,
        w_decay.T,
        head_decay_rate.reshape(1, -1),
        decay_bias.reshape(1, -1),
        head_gain.reshape(1, -1),
        w_proj.reshape(hd, piece),
        ffn_gain.reshape(1, -1),
        w_gate,
        w_up,
        w_down,
    )
    mixed, new_state = pl.pallas_call(
        write_kernel,
        out_shape=(
            jax.ShapeDtypeStruct((rows, piece), bf16),
            jax.ShapeDtypeStruct(state.shape[1:], f32),
        ),
        in_specs=[vmem, vmem],
        out_specs=(hbm, hbm),
        scratch_shapes=[dma((2,))],
        name="write",
    )(*[pltpu.with_memory_space_constraint(x, pltpu.VMEM) for x in (mixed, new_state)])
    return mixed.reshape(hidden.shape), new_state.reshape(state.shape)


def dispatch(nk, nt, hidden, lengths, state, *rest):
    piece, cols = hidden.shape[2], rest[1].shape[1]
    fits = (
        nt == 2
        and nk == 4
        and state.shape[0] == 1
        and hidden.shape[0] % 8 == 0
        and piece % HEAD == 0
        and cols % HEAD == 0
        and rest[-3].shape[1] % HEAD == 0
    )
    plan = functools.partial(fused, nk) if fits else local
    return plan(hidden, lengths, state, *rest)


def solution(mesh):
    in_specs = (
        P("dp", "tp", "kv"),
        P("dp"),
        P(("dp", "kv", "tp"), None, None, None),
        P(),
        P(None, ("kv", "tp")),
        P(None, ("kv", "tp")),
        P(None, ("kv", "tp")),
        P(None, ("kv", "tp")),
        P(),
        P(),
        P(),
        P(),
        P(),
        P(None, "tp", "kv"),
        P(),
        P("tp", "kv"),
        P("tp", "kv"),
        P("kv", "tp"),
    )
    out_specs = (P("dp", "tp", "kv"), P(("dp", "kv", "tp"), None, None, None))
    plan = functools.partial(dispatch, mesh.shape["kv"], mesh.shape["tp"])
    return jax.shard_map(plan, mesh=mesh, in_specs=in_specs, out_specs=out_specs, check_vma=False)
```

```python
import functools

import jax
import jax.numpy as jnp
from jax import lax
from jax.experimental import pallas as pl
from jax.experimental.pallas import tpu as pltpu
from jax.sharding import PartitionSpec as P

D = 4096
HEADS = 16
HEAD = 128
SLOTS = 3


EPS = 1e-06


def recur(loop_carry, query_vector, key, value, beta, logdecay):
    query_scale = query_vector.shape[-1] ** (-0.5)
    output_rows = []
    for state_slot in range(query_vector.shape[0]):
        loop_carry = loop_carry * jnp.exp(logdecay[state_slot])[:, None, None]
        recalled_value = jnp.einsum(
            "jtu,jt->ju", loop_carry, key[state_slot], precision=lax.Precision.HIGHEST
        )
        change = beta[state_slot][:, None] * (value[state_slot] - recalled_value)
        loop_carry = loop_carry + key[state_slot][:, :, None] * change[:, None, :]
        output_rows.append(
            jnp.einsum(
                "jtu,jt->ju", loop_carry, query_vector[state_slot], precision=lax.Precision.HIGHEST
            )
            * query_scale
        )
    return (loop_carry, jnp.stack(output_rows))


def unit_rows(values):
    return values * lax.rsqrt(jnp.sum(values * values, axis=-1, keepdims=True) + EPS)


def local(
    hidden,
    lengths,
    state,
    attn_gain,
    w_query,
    w_key,
    w_value,
    w_outgate,
    w_beta,
    w_decay,
    head_decay_rate,
    decay_bias,
    head_gain,
    w_proj,
    ffn_gain,
    w_gate,
    w_up,
    w_down,
):
    rank = lax.axis_index(("kv", "tp"))
    core = lax.axis_index("tp")
    own = state.shape[0]
    own_rows = own * SLOTS
    row_total = hidden.shape[0]
    piece_cols = hidden.shape[2]
    half_cols = piece_cols * lax.axis_size("kv")
    live = (jnp.arange(SLOTS)[None, :] < lengths[:, None]).astype(jnp.float32).reshape(-1)
    own_lengths = lax.dynamic_slice_in_dim(lengths, rank * own, own)
    own_live = (jnp.arange(SLOTS)[None, :] < own_lengths[:, None]).astype(jnp.float32).reshape(-1)
    half_rows = lax.all_gather(hidden, "kv", axis=2, tiled=True)
    whole = lax.all_gather(half_rows, "tp", axis=1, tiled=True).reshape(row_total, -1)
    xf = whole.astype(jnp.float32)
    normed = (xf * lax.rsqrt(jnp.mean(xf * xf, axis=1, keepdims=True) + EPS) * attn_gain).astype(
        jnp.bfloat16
    )
    projected = jnp.stack(
        [
            jnp.dot(normed, weight, preferred_element_type=jnp.float32)
            for weight in (w_query, w_key, w_value, w_outgate)
        ],
        axis=1,
    ).astype(jnp.bfloat16)
    mine = lax.all_to_all(projected, ("kv", "tp"), split_axis=0, concat_axis=2, tiled=True)
    own_normed = lax.dynamic_slice_in_dim(normed, rank * own_rows, own_rows, 0)
    beta = own_live[:, None] * jax.nn.sigmoid(
        jnp.dot(own_normed, w_beta, preferred_element_type=jnp.float32)
    )
    pre = jnp.dot(own_normed, w_decay, preferred_element_type=jnp.float32)
    logdecay = -own_live[:, None] * head_decay_rate * jax.nn.softplus(pre + decay_bias)
    shape = (own, SLOTS, HEADS, HEAD)
    q_own = unit_rows(mine[:, 0].astype(jnp.float32).reshape(shape))
    k_own = unit_rows(mine[:, 1].astype(jnp.float32).reshape(shape))
    v_own = mine[:, 2].astype(jnp.float32).reshape(shape)
    zf = mine[:, 3].astype(jnp.float32).reshape(shape)
    new_state, out = jax.vmap(recur)(
        state,
        q_own,
        k_own,
        v_own,
        beta.reshape(own, SLOTS, HEADS),
        logdecay.reshape(own, SLOTS, HEADS),
    )
    gated = (
        out
        * lax.rsqrt(jnp.mean(out * out, axis=-1, keepdims=True) + EPS)
        * head_gain
        * jax.nn.silu(zf)
    )
    gated = gated.reshape(own_rows, HEADS * HEAD).astype(jnp.bfloat16)
    proj_cols = w_proj.reshape(w_proj.shape[0], -1)
    mixer = jnp.dot(
        lax.all_gather(gated, ("kv", "tp"), axis=0, tiled=True),
        proj_cols,
        preferred_element_type=jnp.float32,
    )
    stream = (hidden.astype(jnp.float32) + mixer[:, None, :]).astype(jnp.bfloat16)
    sf = stream.astype(jnp.float32)
    half_stream = lax.all_gather(stream, "kv", axis=2, tiled=True)[:, 0, :]
    hf = half_stream.astype(jnp.float32)
    squares = lax.psum(jnp.sum(hf * hf, axis=1), "tp")
    gain_half = lax.dynamic_slice_in_dim(ffn_gain, core * half_cols, half_cols)
    fnormed = (hf * lax.rsqrt(squares / D + EPS)[:, None] * gain_half).astype(jnp.bfloat16)
    gate_part = jnp.dot(fnormed, w_gate, preferred_element_type=jnp.float32)
    up_part = jnp.dot(fnormed, w_up, preferred_element_type=jnp.float32)
    gate, upper = (
        lax.psum(gate_part.astype(jnp.bfloat16), "tp").astype(jnp.float32),
        lax.psum(up_part.astype(jnp.bfloat16), "tp").astype(jnp.float32),
    )
    inner = (jax.nn.silu(gate) * upper).astype(jnp.bfloat16)
    partial_down = jnp.dot(inner, w_down, preferred_element_type=jnp.float32)[:, None, :]
    down = lax.psum_scatter(partial_down, "kv", scatter_dimension=2, tiled=True)
    mixed = ((sf + down) * live[:, None, None]).astype(jnp.bfloat16)
    return (mixed, new_state)


def layer_kernel(
    nk,
    hidden,
    lengths_hbm,
    state_hbm,
    attn_gain_hbm,
    wq_hbm,
    wk_hbm,
    wv_hbm,
    wz_hbm,
    wb_hbm,
    wd_hbm,
    rate_hbm,
    bias_hbm,
    head_gain_hbm,
    wp_hbm,
    ffn_gain_hbm,
    wg_hbm,
    wu_hbm,
    wdn_hbm,
    mixed,
    state_out,
    w_all,
    w_p,
    w_g,
    w_u,
    w_dn,
    w_bd,
    st,
    hx,
    acc,
    blocks,
    scale,
    px,
    rx,
    flat,
    qk,
    qkt,
    outs,
    gx,
    rg,
    flat2,
    sx,
    acc_g,
    acc_u,
    xs,
    rs,
    sq,
    rsq,
    dx,
    rd,
    lengths,
    attn_gain,
    ffn_gain,
    rate,
    bias,
    head_gain,
    w_sem,
    h_send,
    h_recv,
    p_send,
    p_recv,
    g_send,
    g_recv,
    s_send,
    s_recv,
    x_send,
    x_recv,
    d_send,
    d_recv,
):
    f32, bf16 = jnp.float32, jnp.bfloat16
    c = lax.axis_index("kv")
    t = lax.axis_index("tp")
    me = c * 2 + t
    group = 2 * nk
    rows, piece = hidden.shape
    cols = w_p.shape[0] // group
    seqs = rows // SLOTS
    width = group * piece
    turn = 1 - 2 * (c // max(nk // 2, 1))

    def near(i):
        return lax.rem(c + turn * i + nk, nk)

    def send(src, dst, ssem, rsem, kv, tp):
        copy = pltpu.make_async_remote_copy(
            src_ref=src,
            dst_ref=dst,
            send_sem=ssem,
            recv_sem=rsem,
            device_id={"kv": kv, "tp": tp},
            device_id_type=pl.DeviceIdType.MESH,
        )
        copy.start()
        return copy

    def arrived(ref, ssem, rsem):
        pltpu.make_async_remote_copy(
            src_ref=ref,
            dst_ref=ref,
            send_sem=ssem,
            recv_sem=rsem,
            device_id={"kv": c, "tp": 1 - t},
            device_id_type=pl.DeviceIdType.MESH,
        ).wait_recv()

    barrier = pltpu.get_barrier_semaphore()
    others = [(i, j) for i in reversed(range(nk)) for j in range(2) if i or j]
    for i, j in others:
        pl.semaphore_signal(
            barrier,
            inc=1,
            device_id={"kv": near(i), "tp": lax.rem(t + j, 2)},
            device_id_type=pl.DeviceIdType.MESH,
        )
    loads = []

    def load(src, dst):
        copy = pltpu.make_async_copy(src, dst, w_sem.at[len(loads)])
        copy.start()
        loads.append(copy)
        return copy

    own_slot = t * nk + c
    own_off = pl.multiple_of(own_slot * piece, piece)
    load_hidden = load(hidden, hx.at[own_slot])
    load_small = [
        load(a, b)
        for a, b in (
            (attn_gain_hbm, attn_gain),
            (lengths_hbm, lengths),
            (ffn_gain_hbm, ffn_gain),
            (rate_hbm, rate),
            (bias_hbm, bias),
            (head_gain_hbm, head_gain),
        )
    ]
    load_b = load(wb_hbm.at[:, pl.ds(own_off, piece)], w_bd.at[0:HEADS, :])
    load_d = load(wd_hbm.at[:, pl.ds(own_off, piece)], w_bd.at[HEADS : 2 * HEADS, :])
    w_bd[2 * HEADS :, :] = jnp.zeros((HEAD - 2 * HEADS, piece), bf16)
    load_proj = [load(w, w_all.at[j]) for j, w in enumerate((wq_hbm, wk_hbm, wv_hbm, wz_hbm))]
    load_state = load(state_hbm, st)
    load_p = load(wp_hbm, w_p)
    load_gu = [
        [load(a.at[pl.ds(near(i) * piece, piece), :], b.at[pl.ds(near(i) * piece, piece), :])
         for a, b in ((wg_hbm, w_g), (wu_hbm, w_u))]
        for i in range(nk)
    ]
    part = w_dn.shape[0] // 4
    load_dn = [
        load(wdn_hbm.at[pl.ds(i * part, part), :], w_dn.at[pl.ds(i * part, part), :])
        for i in range(4)
    ]

    sends = []
    load_hidden.wait()
    pl.semaphore_wait(barrier, len(others))

    mine = hx.at[own_slot]
    for i in reversed(range(1, nk)):
        sends.append(send(mine, mine, h_send.at[i], h_recv.at[own_slot], near(i), t))
    sends.append(send(mine, mine, h_send.at[0], h_recv.at[own_slot], c, 1 - t))

    def scaled(x, gain_ref, slot):
        gain = gain_ref[:, pl.ds(pl.multiple_of(slot * piece, piece), piece)]
        return (x * gain).astype(bf16)

    def proj(x, slot):
        return [
            jnp.dot(
                x,
                w_all[j, pl.ds(pl.multiple_of(slot * piece, piece), piece), :],
                preferred_element_type=f32,
            )
            for j in range(4)
        ]

    for copy in load_small:
        copy.wait()
    hf = hx[own_slot].astype(f32)
    xg = scaled(hf, attn_gain, own_slot)
    load_b.wait()
    load_d.wait()
    pbd = lax.dot_general(xg, w_bd[...], (((1,), (1,)), ((), ())), preferred_element_type=f32)
    for copy in load_proj:
        copy.wait()
    for j, value in enumerate(proj(xg, own_slot)):
        acc[:, j * cols : (j + 1) * cols] = value
    squares = jnp.sum(hf * hf, axis=1, keepdims=True)

    def slot_step(slot, squares):
        xf = hx[slot].astype(f32)
        for j, value in enumerate(proj(scaled(xf, attn_gain, slot), slot)):
            acc[:, j * cols : (j + 1) * cols] += value
        return squares + jnp.sum(xf * xf, axis=1, keepdims=True)

    for i in range(1, nk):
        slot = t * nk + near(i)
        arrived(hx.at[slot], h_send.at[0], h_recv.at[slot])
        sends.append(
            send(hx.at[slot], hx.at[slot], h_send.at[nk - 1 + i], h_recv.at[slot], c, 1 - t)
        )
        squares = slot_step(slot, squares)

    def partner_step(i, total):
        slot = (1 - t) * nk + near(i)
        arrived(hx.at[slot], h_send.at[0], h_recv.at[slot])
        return slot_step(slot, total)

    squares = lax.fori_loop(0, nk, partner_step, squares)
    rms = lax.rsqrt(squares / width + EPS)
    scale[...] = jnp.broadcast_to(rms, (rows, HEAD))
    per = 4 * cols // HEAD
    for j in range(per):
        blocks[pl.ds(j, rows, stride=per), :] = acc[:, j * HEAD : (j + 1) * HEAD] * rms
    high = pbd.astype(bf16).astype(f32)
    low = pbd - high
    zero = jnp.zeros((2, HEAD), f32)
    span = SLOTS * per
    for g in range(group):
        at = slice(g * SLOTS, (g + 1) * SLOTS)
        px[g, 0:span, :] = blocks[g * span : (g + 1) * span, :].astype(bf16)
        px[g, span : span + 8, :] = jnp.concatenate([high[at], low[at], zero], axis=0).astype(bf16)
    for i, j in others:
        kv, tp = near(i), lax.rem(t + j, 2)
        sends.append(
            send(px.at[kv * 2 + tp], rx.at[me], p_send.at[i * 2 + j], p_recv.at[me], kv, tp)
        )
    rx[me] = px[me]
    tall = span + 8

    own_len = lengths[me]
    own_rms = [scale[pl.ds(me * SLOTS + s, 1), :] for s in range(SLOTS)]
    load_state.wait()
    for i, j in others:
        src = near(i) * 2 + lax.rem(t + j, 2)
        arrived(rx.at[src], p_send.at[0], p_recv.at[src])
    for g in range(group):
        flat[g * tall : (g + 1) * tall, :] = rx[g].astype(f32)
    hh = cols // HEAD

    def tile(s, p, h):
        return flat[pl.ds(s * per + p * hh + h, group, stride=tall), :]

    def unit(x):
        return x * lax.rsqrt(jnp.sum(x * x, axis=1, keepdims=True) + EPS)

    qk[...] = jnp.zeros_like(qk)
    for s in range(SLOTS):
        for h in range(hh):
            at = (s * hh + h) * group
            qk[at : at + group, :] = unit(tile(s, 0, h))
            at += SLOTS * HEADS
            qk[at : at + group, :] = unit(tile(s, 1, h))
    for s in range(SLOTS):
        pre = jnp.sum(
            flat[pl.ds(span + s, group, stride=tall), :]
            + flat[pl.ds(span + SLOTS + s, group, stride=tall), :],
            axis=0,
            keepdims=True,
        ) * own_rms[s]
        live = jnp.where(s < own_len, 1.0, 0.0).astype(f32)
        arg = pre[:, HEADS : 2 * HEADS] + bias[...]
        soft = jnp.maximum(arg, 0.0) + jnp.log1p(jnp.exp(-jnp.abs(arg)))
        at = 2 * SLOTS * HEADS + s
        qk[at : at + 1, 0:HEADS] = live * jax.nn.sigmoid(pre[:, :HEADS])
        qk[at + SLOTS : at + SLOTS + 1, 0:HEADS] = jnp.exp(-live * rate[...] * soft)
    qkt[...] = qk[...].T
    inv = HEAD**-0.5
    many = SLOTS * HEADS

    def start(s, h):
        return (s * hh + h) * group

    for src in range(group):
        for h in range(hh):
            every = pl.ds(start(0, h) + src, 8, stride=HEADS)
            flat2[every, :] = jnp.dot(
                qk[every, :],
                st[src * hh + h],
                precision=lax.Precision.HIGHEST,
                preferred_element_type=f32,
            )

    def dots(x, y):
        return jnp.sum(x * y, axis=1, keepdims=True)

    for h in range(hh):
        per_head = qkt[pl.ds(h, group, stride=hh), :]
        q, k, seen_q, seen_k, w = [], [], [], [], []
        beta = [per_head[:, 2 * many + s : 2 * many + s + 1] for s in range(SLOTS)]
        keep = [
            per_head[:, 2 * many + SLOTS + s : 2 * many + SLOTS + s + 1] for s in range(SLOTS)
        ]
        for s in range(SLOTS):
            at = start(s, h)
            q.append(qk[at : at + group, :])
            k.append(qk[at + many : at + many + group, :])
            seen_q.append(flat2[at : at + group, :])
            seen_k.append(flat2[at + many : at + many + group, :])
        total = jnp.ones((group, 1), f32)
        for s in range(SLOTS):
            total = total * keep[s]
            recalled = total * seen_k[s]
            w = [keep[s] * x for x in w]
            for n in range(s):
                recalled = recalled + dots(k[n], k[s]) * w[n]
            w.append(beta[s] * (tile(s, 2, h) - recalled))
            o = total * seen_q[s]
            for n in range(s + 1):
                o = o + dots(k[n], q[s]) * w[n]
            o = o * inv
            z = tile(s, 3, h)
            at = start(s, h)
            outs[at : at + group, :] = (
                o
                * lax.rsqrt(jnp.mean(o * o, axis=1, keepdims=True) + EPS)
                * head_gain[...]
                * (z * jax.nn.sigmoid(z))
            )
        for s in range(SLOTS):
            at = 2 * many + start(s, h)
            flat2[at : at + group, :] = w[s]
        at = 2 * many + start(SLOTS, h)
        flat2[at : at + group, :] = jnp.broadcast_to(total, (group, HEAD))
    gx[...] = outs[...].astype(bf16)
    for i, j in others:
        kv, tp = near(i), lax.rem(t + j, 2)
        sends.append(send(gx, rg.at[me], g_send.at[i * 2 + j], g_recv.at[me], kv, tp))
    rg[me] = gx[...]
    for src in range(group):
        for h in range(hh):
            at = 2 * many + start(SLOTS, h) + src
            S = st[src * hh + h] * flat2[at : at + 1, :]
            for s in range(SLOTS):
                col = start(s, h) + src + many
                S = S + qkt[:, col : col + 1] * flat2[col + many : col + many + 1, :]
            state_out[src * hh + h] = S
    load_p.wait()
    for i, j in others:
        src = near(i) * 2 + lax.rem(t + j, 2)
        arrived(rg.at[src], g_send.at[0], g_recv.at[src])
    for g in range(group):
        flat2[g * SLOTS * HEADS : (g + 1) * SLOTS * HEADS, :] = rg[g].astype(f32)
    gall = jnp.concatenate(
        [
            flat2[pl.ds((n % hh) * group + n // hh, rows, stride=HEADS), :].astype(bf16)
            for n in range(HEADS)
        ],
        axis=1,
    )
    mixer = jnp.dot(gall, w_p[...], preferred_element_type=f32)
    sx[c] = (hf + mixer).astype(bf16)
    for i in reversed(range(1, nk)):
        sends.append(send(sx.at[c], sx.at[c], s_send.at[i], s_recv.at[c], near(i), t))

    acc_g[...] = jnp.zeros_like(acc_g)
    acc_u[...] = jnp.zeros_like(acc_u)
    for i in range(nk):
        for copy in load_gu[i]:
            copy.wait()

    def ffn_step(i, total):
        slot = near(i)

        @pl.when(i > 0)
        def _():
            arrived(sx.at[slot], s_send.at[0], s_recv.at[slot])

        xf = sx[slot].astype(f32)
        x = scaled(xf, ffn_gain, t * nk + slot)
        at = pl.ds(pl.multiple_of(slot * piece, piece), piece)
        acc_g[...] += jnp.dot(x, w_g[at, :], preferred_element_type=f32)
        acc_u[...] += jnp.dot(x, w_u[at, :], preferred_element_type=f32)
        return total + jnp.sum(xf * xf, axis=1, keepdims=True)

    half = lax.fori_loop(0, nk, ffn_step, jnp.zeros((rows, 1), f32))
    sq[...] = jnp.broadcast_to(half, (rows, HEAD))
    xs[0] = acc_g[...].astype(bf16)
    xs[1] = acc_u[...].astype(bf16)
    x0 = send(sq, rsq, x_send.at[0], x_recv.at[0], c, 1 - t)
    x1 = send(xs, rs, x_send.at[1], x_recv.at[1], c, 1 - t)
    sends += [x0, x1]
    for copy in load_dn:
        copy.wait()
    x0.wait_recv()
    x1.wait_recv()
    fr = lax.rsqrt((half + rsq[:, 0:1]) / width + EPS)
    gate = (acc_g[...] + rs[0].astype(f32)) * fr
    upper = (acc_u[...] + rs[1].astype(f32)) * fr
    inner = (gate * jax.nn.sigmoid(gate) * upper).astype(bf16)
    xs_inner = inner

    def down(slot):
        at = pl.ds(pl.multiple_of(slot * piece, piece), piece)
        return jnp.dot(xs_inner, w_dn[:, at], preferred_element_type=f32)

    for i in range(nk - 1, 0, -1):
        slot = near(i)
        dx[i] = down(slot).astype(bf16)
        sends.append(send(dx.at[i], rd.at[c], d_send.at[i], d_recv.at[c], slot, t))
    total = sx[c].astype(f32) + down(c)
    row = lax.broadcasted_iota(jnp.int32, (rows, piece), 0)
    live = jnp.zeros((rows, piece), f32)
    for n in range(seqs):
        hit = (row >= n * SLOTS) & (row < n * SLOTS + lengths[n])
        live = jnp.where(hit, 1.0, live)
    for i in range(1, nk):
        slot = near(i)
        arrived(rd.at[slot], d_send.at[0], d_recv.at[slot])
        total = total + rd[slot].astype(f32)
    mixed[...] = (total * live).astype(bf16)
    for copy in sends:
        copy.wait_send()


def write_kernel(a, b, a_out, b_out, sem):
    copies = [
        pltpu.make_async_copy(x, y, sem.at[n]) for n, (x, y) in enumerate(((b, b_out), (a, a_out)))
    ]
    for copy in copies:
        copy.start()
    for copy in copies:
        copy.wait()


def fused(
    nk,
    hidden,
    lengths,
    state,
    attn_gain,
    w_query,
    w_key,
    w_value,
    w_outgate,
    w_beta,
    w_decay,
    head_decay_rate,
    decay_bias,
    head_gain,
    w_proj,
    ffn_gain,
    w_gate,
    w_up,
    w_down,
):
    f32, bf16 = jnp.float32, jnp.bfloat16
    rows, _, piece = hidden.shape
    group = 2 * nk
    depth, cols = w_query.shape
    hd = w_proj.shape[0]
    half, ff = w_gate.shape
    per = 4 * cols // HEAD
    tall = SLOTS * per + 8
    vmem = pl.BlockSpec(memory_space=pltpu.VMEM)
    hbm = pl.BlockSpec(memory_space=pl.ANY)
    dma = pltpu.SemaphoreType.DMA
    mixed, new_state = pl.pallas_call(
        functools.partial(layer_kernel, nk),
        out_shape=(
            pltpu.VMEM((rows, piece), bf16),
            pltpu.VMEM(state.shape[1:], f32),
        ),
        in_specs=[hbm] * 18,
        out_specs=(vmem, vmem),
        scratch_shapes=[
            pltpu.VMEM((4, depth, cols), bf16),
            pltpu.VMEM((hd, piece), bf16),
            pltpu.VMEM((half, ff), bf16),
            pltpu.VMEM((half, ff), bf16),
            pltpu.VMEM(w_down.shape, bf16),
            pltpu.VMEM((HEAD, piece), bf16),
            pltpu.VMEM(state.shape[1:], f32),
            pltpu.VMEM((group, rows, piece), bf16),
            pltpu.VMEM((rows, 4 * cols), f32),
            pltpu.VMEM((rows * per, HEAD), f32),
            pltpu.VMEM((rows, HEAD), f32),
            pltpu.VMEM((group, tall, HEAD), bf16),
            pltpu.VMEM((group, tall, HEAD), bf16),
            pltpu.VMEM((group * tall, HEAD), f32),
            pltpu.VMEM((HEAD, HEAD), f32),
            pltpu.VMEM((HEAD, HEAD), f32),
            pltpu.VMEM((SLOTS * HEADS, HEAD), f32),
            pltpu.VMEM((SLOTS * HEADS, HEAD), bf16),
            pltpu.VMEM((group, SLOTS * HEADS, HEAD), bf16),
            pltpu.VMEM((group * SLOTS * HEADS, HEAD), f32),
            pltpu.VMEM((nk, rows, piece), bf16),
            pltpu.VMEM((rows, ff), f32),
            pltpu.VMEM((rows, ff), f32),
            pltpu.VMEM((2, rows, ff), bf16),
            pltpu.VMEM((2, rows, ff), bf16),
            pltpu.VMEM((rows, HEAD), f32),
            pltpu.VMEM((rows, HEAD), f32),
            pltpu.VMEM((nk, rows, piece), bf16),
            pltpu.VMEM((nk, rows, piece), bf16),
            pltpu.SMEM(lengths.shape, jnp.int32),
            pltpu.VMEM((1, 2 * half), f32),
            pltpu.VMEM((1, 2 * half), f32),
            pltpu.VMEM((1, HEADS), f32),
            pltpu.VMEM((1, HEADS), f32),
            pltpu.VMEM((1, HEAD), f32),
            dma((20 + 2 * nk,)),
            dma((group,)),
            dma((group,)),
            dma((group,)),
            dma((group,)),
            dma((group,)),
            dma((group,)),
            dma((nk,)),
            dma((nk,)),
            dma((2,)),
            dma((2,)),
            dma((nk,)),
            dma((nk,)),
        ],
        compiler_params=pltpu.CompilerParams(
            collective_id=0, has_side_effects=True, vmem_limit_bytes=60 * 2**20
        ),
        name="layer",
    )(
        hidden.reshape(rows, piece),
        lengths,
        state.reshape(state.shape[1:]),
        attn_gain.reshape(1, -1),
        w_query,
        w_key,
        w_value,
        w_outgate,
        w_beta.T,
        w_decay.T,
        head_decay_rate.reshape(1, -1),
        decay_bias.reshape(1, -1),
        head_gain.reshape(1, -1),
        w_proj.reshape(hd, piece),
        ffn_gain.reshape(1, -1),
        w_gate,
        w_up,
        w_down,
    )
    mixed, new_state = pl.pallas_call(
        write_kernel,
        out_shape=(
            jax.ShapeDtypeStruct((rows, piece), bf16),
            jax.ShapeDtypeStruct(state.shape[1:], f32),
        ),
        in_specs=[vmem, vmem],
        out_specs=(hbm, hbm),
        scratch_shapes=[dma((2,))],
        name="write",
    )(*[pltpu.with_memory_space_constraint(x, pltpu.VMEM) for x in (mixed, new_state)])
    return mixed.reshape(hidden.shape), new_state.reshape(state.shape)


def dispatch(nk, nt, hidden, lengths, state, *rest):
    piece, cols = hidden.shape[2], rest[1].shape[1]
    fits = (
        nt == 2
        and nk == 4
        and state.shape[0] == 1
        and hidden.shape[0] % 8 == 0
        and piece % HEAD == 0
        and cols % HEAD == 0
        and rest[-3].shape[1] % HEAD == 0
    )
    plan = functools.partial(fused, nk) if fits else local
    return plan(hidden, lengths, state, *rest)


def solution(mesh):
    in_specs = (
        P("dp", "tp", "kv"),
        P("dp"),
        P(("dp", "kv", "tp"), None, None, None),
        P(),
        P(None, ("kv", "tp")),
        P(None, ("kv", "tp")),
        P(None, ("kv", "tp")),
        P(None, ("kv", "tp")),
        P(),
        P(),
        P(),
        P(),
        P(),
        P(None, "tp", "kv"),
        P(),
        P("tp", "kv"),
        P("tp", "kv"),
        P("kv", "tp"),
    )
    out_specs = (P("dp", "tp", "kv"), P(("dp", "kv", "tp"), None, None, None))
    plan = functools.partial(dispatch, mesh.shape["kv"], mesh.shape["tp"])
    return jax.shard_map(plan, mesh=mesh, in_specs=in_specs, out_specs=out_specs, check_vma=False)
```
